256 devices in a mesh: fs: 64 (over z, y, core), tp: 4 (over x).
Axes of the slice: x: 4, y: 4, z: 8, core: 2. Of those that a mesh axis runs over, the one named last changes fastest.
Arguments:
- later_gate: bfloat16 [40960, 5632], P('fs', 'tp'), may hold values from -6 to 6
- later_up: bfloat16 [40960, 5632], P('fs', 'tp'), may hold values from -6 to 6
- early_gate: bfloat16 [40960, 5632], P('fs', 'tp'), may hold values from -6 to 6
- early_up: bfloat16 [40960, 5632], P('fs', 'tp'), may hold values from -6 to 6
- early_cotangent: bfloat16 [40960, 2048], P(('fs', 'tp')), may hold values from -24 to 24
- down_weight: bfloat16 [5632, 2048], P('tp', 'fs'), may hold values from -0.078125 to 0.078125
- grad_running: float32 [5632, 2048], P('tp', 'fs'), may hold values from -640 to 640
Outputs:
- mixed: bfloat16 [40960, 2048], P(('fs', 'tp'))
- gate_grad: bfloat16 [40960, 5632], P('fs', 'tp')
- up_grad: bfloat16 [40960, 5632], P('fs', 'tp')
- grad_total: float32 [5632, 2048], P('tp', 'fs')
The draws below stay inside these ranges and needn't reach their ends.
All inputs are finite; a program needn't handle non-finite values.
Results may differ from the reference program's by a relative error of at most 0.009.
Values may be sent and summed in bfloat16 or wider, within the bound.
No kernel may reach another device: no remote copies, remote signals or barrier semaphores. Data moves between devices by JAX's collectives and lax.ppermute only.
A program may use at most 128 MiB of HBM per device.

```python
import jax
import jax.numpy as jnp

D = 2048
FF = 5632
TOKENS = 40960
N_TP = 4


def raised(entries, own_key, source, target, shards_of, factor):
    owner, partner = [(jnp.arange(entries.shape[dim]) // (entries.shape[dim] // shards_of)).reshape([-1 if axis == dim else 1 for axis in range(entries.ndim)]) for dim in (source, target)]
    chosen = jax.random.permutation(own_key, shards_of)[partner]
    strong = (owner == chosen) | (owner == (partner + shards_of // 2) % shards_of)
    return jnp.where(strong, factor * entries, entries)


def steps_of(rng, extent, pieces, least, top_value):
    factor_of, own = 1.0, jax.random.fold_in(rng, 6)
    for axis_at, shards_of in pieces:
        steps = jnp.exp(jax.random.uniform(jax.random.fold_in(own, axis_at), (shards_of,), jnp.float32, least / len(pieces), top_value / len(pieces)))
        factor_of = factor_of * jnp.repeat(steps, extent[axis_at] // shards_of).reshape([-1 if axis == axis_at else 1 for axis in range(len(extent))])
    return factor_of


def centred(rng, shape, width, reach, shards=(), kind=jnp.bfloat16):
    values = jax.random.normal(rng, shape, jnp.float32) * width
    if len(shards) > 0:
        values = steps_of(rng, shape, shards, -0.22, 0.18) * values
    return jnp.clip(values, min=-reach, max=reach).astype(kind)


def bell_draw_with(own_key, shape, spread, most, cuts, heavy, dtype=jnp.bfloat16):
    drawn = spread * jax.random.normal(own_key, shape, jnp.float32)
    if cuts:
        drawn = drawn * steps_of(own_key, shape, cuts, -0.22, 0.18)
    return jnp.clip(raised(drawn, jax.random.fold_in(own_key, 3), *heavy), -most, most).astype(dtype)


def setup_inputs(seed: int = 0) -> dict:
    key_list = jax.random.split(jax.random.key(seed), 8)
    return {
        "later_gate": centred(key_list[0], (TOKENS, FF), 1.0, 6.0, ((0, 64), (1, 4))),
        "later_up": centred(key_list[1], (TOKENS, FF), 1.0, 6.0, ((0, 64), (1, 4))),
        "early_gate": centred(key_list[2], (TOKENS, FF), 1.0, 6.0, ((0, 64), (1, 4))),
        "early_up": centred(key_list[3], (TOKENS, FF), 1.0, 6.0, ((0, 64), (1, 4))),
        "early_cotangent": bell_draw_with(key_list[4], (TOKENS, D), 1.0, 24.0, ((0, 256),), (0, 1, 256, 6.0)),
        "down_weight": centred(key_list[5], (FF, D), FF ** -0.5, 0.078125, ((0, 4), (1, 64))),
        "grad_running": centred(key_list[6], (FF, D), (0.5 * TOKENS ** 0.5), 640.0, ((0, 4), (1, 64)), jnp.float32),
    }


def reference(later_gate, later_up, early_gate, early_up, early_cotangent, down_weight, grad_running):
    later_hidden = (jax.nn.silu(later_gate.astype(jnp.float32)) * later_up.astype(jnp.float32)).astype(jnp.bfloat16)
    block = FF // N_TP
    total = jnp.zeros((later_hidden.shape[0], D), jnp.float32)
    for index in range(N_TP):
        part = jnp.dot(later_hidden[:, index * block:(index + 1) * block], down_weight[index * block:(index + 1) * block], preferred_element_type=jnp.float32)
        total = total + part.astype(jnp.bfloat16).astype(jnp.float32)
    mixed = total.astype(jnp.bfloat16)
    gate_value = early_gate.astype(jnp.float32)
    up_value = early_up.astype(jnp.float32)
    sigma = jax.nn.sigmoid(gate_value)
    early_hidden = (gate_value * sigma * up_value).astype(jnp.bfloat16)
    hidden_cot = jnp.dot(early_cotangent, down_weight.T, preferred_element_type=jnp.float32)
    gate_grad = (hidden_cot * up_value * sigma * (1.0 + gate_value * (1.0 - sigma))).astype(jnp.bfloat16)
    up_grad = (hidden_cot * gate_value * sigma).astype(jnp.bfloat16)
    grad_total = grad_running + jnp.dot(early_hidden.T, early_cotangent, preferred_element_type=jnp.float32)
    return (mixed, gate_grad, up_grad, grad_total)
```

```python
import jax
import jax.numpy as jnp
from jax import lax
from jax.experimental import pallas as pl
from jax.experimental.pallas import tpu as pltpu
from jax.sharding import PartitionSpec as P


BF = jnp.bfloat16
F32 = jnp.float32
NZ, NY, NC, NX = 8, 4, 2, 4


def fs_id(z, y, c):
    return (z % NZ) * (NY * NC) + (y % NY) * NC + c % NC


def grad_term(where, cot, hidden):
    n, d = cot.shape
    ff = hidden.shape[1]
    w = d // (NZ * NY * NC)
    zs = 2
    tile = zs * NY * NC * w

    def body(where, cot, hidden, give, keep):
        y, c = where[1], where[2]
        tile_term = lax.dot_general(
            cot[...], hidden[...], (((0,), (0,)), ((), ())), preferred_element_type=F32
        ).reshape(zs, NY, NC, w, ff)
        early = pl.program_id(0) * zs < NZ // 2
        for i in range(NY):
            yr = lax.rem(i - y + NY, NY)
            first = jnp.where(yr == 1, 2, jnp.where(yr == 2, 0, 1))
            last = jnp.where(yr == 1, 0, jnp.where(yr == 2, 1, 2))
            slot = jnp.where(yr == 0, 3, jnp.where(early, first, last))
            for j in range(zs):
                zero, one = tile_term[j, i, 0], tile_term[j, i, 1]
                keep[slot, j] = jnp.where(c == 0, zero, one).astype(BF)
                give[slot, j] = jnp.where(c == 0, one, zero).astype(BF)

    def out_index(i, where):
        return (0, i, 0, 0)

    return pl.pallas_call(
        body,
        grid_spec=pltpu.PrefetchScalarGridSpec(
            num_scalar_prefetch=1,
            grid=(NZ // zs,),
            in_specs=[
                pl.BlockSpec((n, tile), lambda i, where: (0, i)),
                pl.BlockSpec((n, ff), lambda i, where: (0, 0)),
            ],
            out_specs=[
                pl.BlockSpec((NY, zs, w, ff), out_index),
                pl.BlockSpec((NY, zs, w, ff), out_index),
            ],
        ),
        out_shape=[
            jax.ShapeDtypeStruct((NY, NZ, w, ff), BF),
            jax.ShapeDtypeStruct((NY, NZ, w, ff), BF),
        ],
        compiler_params=pltpu.CompilerParams(dimension_semantics=("arbitrary",)),
        cost_estimate=pl.CostEstimate(
            flops=2 * n * d * ff, bytes_accessed=12 * 1024 * 1024, transcendentals=0
        ),
        name="grad_term",
    )(where, cot, hidden)


def partial_products(where, hidden, own, other):
    parts, rows, ff = hidden.shape
    count = len(own)
    w = own[0][0].shape[1]
    tile = NY * NC * w
    d = count * tile
    pieces, places = [], []
    for cr, blocks in enumerate((own, other)):
        for zr, block in enumerate(blocks):
            yr = 0
            for piece in block:
                for j in range(piece.shape[0]):
                    places.append((zr, cr, yr, len(pieces), j))
                    yr += 1
                pieces.append(piece)
    n = len(pieces)

    def body(where, hidden, *refs):
        blocks = refs[:n]
        outs, whole = refs[n : n + parts], refs[n + parts]
        ordered, weight, sems = refs[n + parts + 1 :]
        step = pl.program_id(0)
        y, c, t = where[1], where[2], where[3]

        def copies(at):
            return [
                pltpu.make_async_copy(
                    blocks[i].at[j],
                    weight.at[zr, lax.rem(y + yr, NY), lax.rem(c + cr, NC)],
                    sems.at[zr, cr, yr],
                )
                for zr, cr, yr, i, j in places
                if zr == at
            ]

        @pl.when(step == 0)
        def _():
            for zr in range(count):
                for copy in copies(zr):
                    copy.start()
            for i in range(parts):
                ordered[pl.ds(i * rows, rows), :] = hidden[lax.rem(t + i, parts)]

        for zr in range(count):

            @pl.when(step == zr)
            def _(zr=zr):
                for copy in copies(zr):
                    copy.wait()

        part = lax.dot_general(
            ordered[...],
            weight[step].reshape(tile, ff),
            (((1,), (1,)), ((), ())),
            preferred_element_type=F32,
        ).astype(BF)
        for i in range(parts):
            outs[i][...] = part[i * rows : (i + 1) * rows]
        whole[0] = weight[step]

    def at(i, where):
        return lax.rem(i + where[0], NZ)

    return pl.pallas_call(
        body,
        grid_spec=pltpu.PrefetchScalarGridSpec(
            num_scalar_prefetch=1,
            grid=(count,),
            in_specs=[pl.BlockSpec((parts, rows, ff), lambda i, where: (0, 0, 0))]
            + [pl.BlockSpec(memory_space=pltpu.HBM)] * n,
            out_specs=[pl.BlockSpec((rows, tile), lambda i, where: (0, at(i, where)))]
            * parts
            + [
                pl.BlockSpec(
                    (1, NY, NC, w, ff), lambda i, where: (at(i, where), 0, 0, 0, 0)
                )
            ],
            scratch_shapes=[
                pltpu.VMEM((parts * rows, ff), BF),
                pltpu.VMEM((count, NY, NC, w, ff), BF),
                pltpu.SemaphoreType.DMA((count, NC, NY)),
            ],
        ),
        out_shape=[jax.ShapeDtypeStruct((rows, d), BF)] * parts
        + [jax.ShapeDtypeStruct((count, NY, NC, w, ff), BF)],
        compiler_params=pltpu.CompilerParams(dimension_semantics=("arbitrary",)),
        cost_estimate=pl.CostEstimate(
            flops=2 * parts * rows * d * ff,
            bytes_accessed=16 * 1024 * 1024,
            transcendentals=0,
        ),
        name="partial_products",
    )(where, hidden, *pieces)


def pick(x, i, n):
    return lax.dynamic_index_in_dim(x, i % n, 0, keepdims=False)


def shift(x, dz=0, dy=0, dc=0):
    perm = [
        (fs_id(z, y, c), fs_id(z + dz, y + dy, c + dc))
        for z in range(NZ)
        for y in range(NY)
        for c in range(NC)
    ]
    return lax.ppermute(x, "fs", perm)


def shift_x(x, d):
    return lax.ppermute(x, "tp", [(i, (i + d) % NX) for i in range(NX)])


def step(
    later_gate, later_up, early_gate, early_up, early_cotangent, down_weight, grad_running
):
    k = lax.axis_index("fs")
    t = lax.axis_index("tp")
    where = jnp.stack([k // (NY * NC), (k // NC) % NY, k % NC, t]).astype(jnp.int32)
    rows, d = early_cotangent.shape
    ff, _ = down_weight.shape

    h = rows // 2
    cot = early_cotangent
    from_m = shift_x(cot, 1)
    from_p = shift_x(cot, -1)
    far_top = shift_x(from_m[:h], 1)
    far_bot = shift_x(from_p[h:], -1)
    cot_rows = jnp.zeros((NX, rows, d), BF)

    def put(buf, x, i, j=0):
        return lax.dynamic_update_slice(buf, x[None], ((t + i) % NX, j, 0))

    cot_rows = put(cot_rows, cot, 0)
    cot_rows = put(cot_rows, from_p, 1)
    cot_rows = put(cot_rows, from_m, 3)
    cot_rows = put(cot_rows, far_top, 2)
    cot_rows = put(cot_rows, far_bot, 2, h).reshape(NX * rows, d)

    later_hidden = (
        jax.nn.silu(later_gate.astype(F32)) * later_up.astype(F32)
    ).astype(BF)
    gate_value = early_gate.astype(F32)
    up_value = early_up.astype(F32)
    sigma = jax.nn.sigmoid(gate_value)
    early = lax.optimization_barrier((early_gate, early_up))
    early_hidden = (jax.nn.silu(early[0].astype(F32)) * early[1].astype(F32)).astype(BF)

    w0 = down_weight.T
    wy = jnp.stack([w0, shift(w0, dy=-1), shift(w0, dy=2), shift(w0, dy=1)])
    up1, dn1 = shift(wy, dz=1), shift(wy, dz=-1)
    c0 = shift(wy, dc=1)
    up2, dn2 = shift(up1, dz=1), shift(dn1, dz=-1)
    c1, c7 = shift(dn1, dc=1), shift(up1, dc=1)

    give, keep = grad_term(where, cot_rows, early_hidden)
    came = shift(give, dc=1)
    up_y, dn_y, fwd_y, own_y = (
        keep[i].astype(F32) + came[i].astype(F32) for i in range(NY)
    )

    up3, dn3 = shift(up2, dz=1), shift(dn2, dz=-1)
    c2, c6 = shift(dn2, dc=1), shift(up2, dc=1)

    q = NZ // 2
    up = shift(up_y.astype(BF), dy=1)
    dn = shift(dn_y.astype(BF), dy=-1)

    far = shift(up3, dz=1)
    c3, c5 = shift(dn3, dc=1), shift(up3, dc=1)
    c4 = shift(far, dc=1)
    own = [[wy], [dn1], [dn2], [dn3], [far], [up3], [up2], [up1]]
    other = [[c0], [c1], [c2], [c3], [c4], [c5], [c6], [c7]]

    up2y = shift((fwd_y[:q] + up[:q].astype(F32)).astype(BF), dy=1)
    dn2y = shift((fwd_y[q:] + dn[q:].astype(F32)).astype(BF), dy=-1)
    first = own_y[:q] + dn[:q].astype(F32) + up2y.astype(F32)
    last = own_y[q:] + up[q:].astype(F32) + dn2y.astype(F32)
    reduced = jnp.concatenate([first, last]).astype(BF)
    summed = pick(reduced, where[0], NZ).astype(F32)
    for i in (4, 3, 5, 2, 6, 1, 7):
        block = pick(reduced, where[0] + i, NZ)
        summed = summed + shift(block, dz=i).astype(F32)
    grad_total = grad_running + summed.T

    p0, p1, p2, p3, whole = partial_products(
        where, later_hidden.reshape(NX, rows, ff), own, other
    )
    total = p0.astype(F32)
    for i, p in ((2, p2), (1, p1), (3, p3)):
        total = total + shift_x(p, i).astype(F32)
    mixed = total.astype(BF)

    hidden_cot = jnp.dot(
        cot_rows, whole.reshape(d, ff), preferred_element_type=F32
    )
    gate_grad = (
        hidden_cot * up_value * sigma * (1.0 + gate_value * (1.0 - sigma))
    ).astype(BF)
    up_grad = (hidden_cot * gate_value * sigma).astype(BF)
    return (mixed, gate_grad, up_grad, grad_total)


def solution(mesh):
    placed = (
        P("fs", "tp"),
        P("fs", "tp"),
        P("fs", "tp"),
        P("fs", "tp"),
        P(("fs", "tp"), None),
        P("tp", "fs"),
        P("tp", "fs"),
    )
    return jax.shard_map(
        step,
        mesh=mesh,
        in_specs=placed,
        out_specs=(P(("fs", "tp"), None), P("fs", "tp"), P("fs", "tp"), P("tp", "fs")),
        check_vma=False,
    )
```

```python
import jax
import jax.numpy as jnp
from jax import lax
from jax.experimental import pallas as pl
from jax.experimental.pallas import tpu as pltpu
from jax.sharding import PartitionSpec as P


BF = jnp.bfloat16
F32 = jnp.float32
NZ, NY, NC, NX = 8, 4, 2, 4


def fs_id(z, y, c):
    return (z % NZ) * (NY * NC) + (y % NY) * NC + c % NC


def grad_term(where, cot, hidden):
    n, d = cot.shape
    ff = hidden.shape[1]
    w = d // (NZ * NY * NC)
    zs = 2
    tile = zs * NY * NC * w

    def body(where, cot, hidden, give, keep):
        y, c = where[1], where[2]
        tile_term = lax.dot_general(
            cot[...], hidden[...], (((0,), (0,)), ((), ())), preferred_element_type=F32
        ).reshape(zs, NY, NC, w, ff)
        early = pl.program_id(0) * zs < NZ // 2
        for i in range(NY):
            yr = lax.rem(i - y + NY, NY)
            first = jnp.where(yr == 1, 2, jnp.where(yr == 2, 0, 1))
            last = jnp.where(yr == 1, 0, jnp.where(yr == 2, 1, 2))
            slot = jnp.where(yr == 0, 3, jnp.where(early, first, last))
            for j in range(zs):
                zero, one = tile_term[j, i, 0], tile_term[j, i, 1]
                keep[slot, j] = jnp.where(c == 0, zero, one).astype(BF)
                give[slot, j] = jnp.where(c == 0, one, zero).astype(BF)

    def out_index(i, where):
        return (0, i, 0, 0)

    return pl.pallas_call(
        body,
        grid_spec=pltpu.PrefetchScalarGridSpec(
            num_scalar_prefetch=1,
            grid=(NZ // zs,),
            in_specs=[
                pl.BlockSpec((n, tile), lambda i, where: (0, i)),
                pl.BlockSpec((n, ff), lambda i, where: (0, 0)),
            ],
            out_specs=[
                pl.BlockSpec((NY, zs, w, ff), out_index),
                pl.BlockSpec((NY, zs, w, ff), out_index),
            ],
        ),
        out_shape=[
            jax.ShapeDtypeStruct((NY, NZ, w, ff), BF),
            jax.ShapeDtypeStruct((NY, NZ, w, ff), BF),
        ],
        compiler_params=pltpu.CompilerParams(
            dimension_semantics=("arbitrary",), vmem_limit_bytes=24 * 1024 * 1024
        ),
        cost_estimate=pl.CostEstimate(
            flops=2 * n * d * ff, bytes_accessed=12 * 1024 * 1024, transcendentals=0
        ),
        name="grad_term",
    )(where, cot, hidden)


def partial_products(where, hidden, own, other):
    parts, rows, ff = hidden.shape
    count = len(own)
    w = own[0][0].shape[1]
    tile = NY * NC * w
    d = count * tile
    pieces, places = [], []
    for cr, blocks in enumerate((own, other)):
        for zr, block in enumerate(blocks):
            yr = 0
            for piece in block:
                for j in range(piece.shape[0]):
                    places.append((zr, cr, yr, len(pieces), j))
                    yr += 1
                pieces.append(piece)
    n = len(pieces)

    def body(where, hidden, *refs):
        blocks = refs[:n]
        outs, whole = refs[n : n + parts], refs[n + parts]
        ordered, weight, sems = refs[n + parts + 1 :]
        step = pl.program_id(0)
        y, c, t = where[1], where[2], where[3]

        def copies(at):
            return [
                pltpu.make_async_copy(
                    blocks[i].at[j],
                    weight.at[zr, lax.rem(y + yr, NY), lax.rem(c + cr, NC)],
                    sems.at[zr, cr, yr],
                )
                for zr, cr, yr, i, j in places
                if zr == at
            ]

        @pl.when(step == 0)
        def _():
            for zr in range(count):
                for copy in copies(zr):
                    copy.start()
            for i in range(parts):
                ordered[pl.ds(i * rows, rows), :] = hidden[lax.rem(t + i, parts)]

        for zr in range(count):

            @pl.when(step == zr)
            def _(zr=zr):
                for copy in copies(zr):
                    copy.wait()

        part = lax.dot_general(
            ordered[...],
            weight[step].reshape(tile, ff),
            (((1,), (1,)), ((), ())),
            preferred_element_type=F32,
        ).astype(BF)
        for i in range(parts):
            outs[i][...] = part[i * rows : (i + 1) * rows]
        whole[0] = weight[step]

    def at(i, where):
        return lax.rem(i + where[0], NZ)

    return pl.pallas_call(
        body,
        grid_spec=pltpu.PrefetchScalarGridSpec(
            num_scalar_prefetch=1,
            grid=(count,),
            in_specs=[pl.BlockSpec((parts, rows, ff), lambda i, where: (0, 0, 0))]
            + [pl.BlockSpec(memory_space=pltpu.HBM)] * n,
            out_specs=[pl.BlockSpec((rows, tile), lambda i, where: (0, at(i, where)))]
            * parts
            + [
                pl.BlockSpec(
                    (1, NY, NC, w, ff), lambda i, where: (at(i, where), 0, 0, 0, 0)
                )
            ],
            scratch_shapes=[
                pltpu.VMEM((parts * rows, ff), BF),
                pltpu.VMEM((count, NY, NC, w, ff), BF),
                pltpu.SemaphoreType.DMA((count, NC, NY)),
            ],
        ),
        out_shape=[jax.ShapeDtypeStruct((rows, d), BF)] * parts
        + [jax.ShapeDtypeStruct((count, NY, NC, w, ff), BF)],
        compiler_params=pltpu.CompilerParams(
            dimension_semantics=("arbitrary",), vmem_limit_bytes=24 * 1024 * 1024
        ),
        cost_estimate=pl.CostEstimate(
            flops=2 * parts * rows * d * ff,
            bytes_accessed=16 * 1024 * 1024,
            transcendentals=0,
        ),
        name="partial_products",
    )(where, hidden, *pieces)


def pick(x, i, n):
    return lax.dynamic_index_in_dim(x, i % n, 0, keepdims=False)


def shift(x, dz=0, dy=0, dc=0):
    perm = [
        (fs_id(z, y, c), fs_id(z + dz, y + dy, c + dc))
        for z in range(NZ)
        for y in range(NY)
        for c in range(NC)
    ]
    return lax.ppermute(x, "fs", perm)


def shift_x(x, d):
    return lax.ppermute(x, "tp", [(i, (i + d) % NX) for i in range(NX)])


def step(
    later_gate, later_up, early_gate, early_up, early_cotangent, down_weight, grad_running
):
    k = lax.axis_index("fs")
    t = lax.axis_index("tp")
    where = jnp.stack([k // (NY * NC), (k // NC) % NY, k % NC, t]).astype(jnp.int32)
    rows, d = early_cotangent.shape
    ff, _ = down_weight.shape

    h = rows // 2
    cot = early_cotangent
    from_m = shift_x(cot, 1)
    from_p = shift_x(cot, -1)
    far_top = shift_x(from_m[:h], 1)
    far_bot = shift_x(from_p[h:], -1)
    cot_rows = jnp.zeros((NX, rows, d), BF)

    def put(buf, x, i, j=0):
        return lax.dynamic_update_slice(buf, x[None], ((t + i) % NX, j, 0))

    cot_rows = put(cot_rows, cot, 0)
    cot_rows = put(cot_rows, from_p, 1)
    cot_rows = put(cot_rows, from_m, 3)
    cot_rows = put(cot_rows, far_top, 2)
    cot_rows = put(cot_rows, far_bot, 2, h).reshape(NX * rows, d)

    later_hidden = (
        jax.nn.silu(later_gate.astype(F32)) * later_up.astype(F32)
    ).astype(BF)
    gate_value = early_gate.astype(F32)
    up_value = early_up.astype(F32)
    sigma = jax.nn.sigmoid(gate_value)
    early = lax.optimization_barrier((early_gate, early_up))
    early_hidden = (jax.nn.silu(early[0].astype(F32)) * early[1].astype(F32)).astype(BF)

    w0 = down_weight.T
    wy = jnp.stack([w0, shift(w0, dy=-1), shift(w0, dy=2), shift(w0, dy=1)])
    up1, dn1 = shift(wy, dz=1), shift(wy, dz=-1)
    c0 = shift(wy, dc=1)
    up2, dn2 = shift(up1, dz=1), shift(dn1, dz=-1)
    c1, c7 = shift(dn1, dc=1), shift(up1, dc=1)

    give, keep = grad_term(where, cot_rows, early_hidden)
    came = shift(give, dc=1)
    up_y, dn_y, fwd_y, own_y = (
        keep[i].astype(F32) + came[i].astype(F32) for i in range(NY)
    )

    up3, dn3 = shift(up2, dz=1), shift(dn2, dz=-1)
    c2, c6 = shift(dn2, dc=1), shift(up2, dc=1)

    q = NZ // 2
    up = shift(up_y.astype(BF), dy=1)
    dn = shift(dn_y.astype(BF), dy=-1)

    far = shift(up3, dz=1)
    c3, c5 = shift(dn3, dc=1), shift(up3, dc=1)
    c4 = shift(far, dc=1)
    own = [[wy], [dn1], [dn2], [dn3], [far], [up3], [up2], [up1]]
    other = [[c0], [c1], [c2], [c3], [c4], [c5], [c6], [c7]]

    up2y = shift((fwd_y[:q] + up[:q].astype(F32)).astype(BF), dy=1)
    dn2y = shift((fwd_y[q:] + dn[q:].astype(F32)).astype(BF), dy=-1)
    first = own_y[:q] + dn[:q].astype(F32) + up2y.astype(F32)
    last = own_y[q:] + up[q:].astype(F32) + dn2y.astype(F32)
    reduced = jnp.concatenate([first, last]).astype(BF)
    summed = pick(reduced, where[0], NZ).astype(F32)
    for i in (4, 3, 5, 2, 6, 1, 7):
        block = pick(reduced, where[0] + i, NZ)
        summed = summed + shift(block, dz=i).astype(F32)
    grad_total = grad_running + summed.T

    p0, p1, p2, p3, whole = partial_products(
        where, later_hidden.reshape(NX, rows, ff), own, other
    )
    total = p0.astype(F32)
    for i, p in ((2, p2), (1, p1), (3, p3)):
        total = total + shift_x(p, i).astype(F32)
    mixed = total.astype(BF)

    hidden_cot = jnp.dot(
        cot_rows, whole.reshape(d, ff), preferred_element_type=F32
    )
    gate_grad = (
        hidden_cot * up_value * sigma * (1.0 + gate_value * (1.0 - sigma))
    ).astype(BF)
    up_grad = (hidden_cot * gate_value * sigma).astype(BF)
    return (mixed, gate_grad, up_grad, grad_total)


def solution(mesh):
    placed = (
        P("fs", "tp"),
        P("fs", "tp"),
        P("fs", "tp"),
        P("fs", "tp"),
        P(("fs", "tp"), None),
        P("tp", "fs"),
        P("tp", "fs"),
    )
    return jax.shard_map(
        step,
        mesh=mesh,
        in_specs=placed,
        out_specs=(P(("fs", "tp"), None), P("fs", "tp"), P("fs", "tp"), P("tp", "fs")),
        check_vma=False,
    )
```

```python
import jax
import jax.numpy as jnp
from jax import lax
from jax.experimental import pallas as pl
from jax.experimental.pallas import tpu as pltpu
from jax.sharding import PartitionSpec as P


BF = jnp.bfloat16
F32 = jnp.float32
NZ, NY, NC, NX = 8, 4, 2, 4


def fs_id(z, y, c):
    return (z % NZ) * (NY * NC) + (y % NY) * NC + c % NC


def grad_term(where, cot, hidden):
    n, d = cot.shape
    ff = hidden.shape[1]
    w = d // (NZ * NY * NC)
    zs = 2
    tile = zs * NY * NC * w

    def body(where, cot, hidden, give, keep):
        y, c = where[1], where[2]
        tile_term = lax.dot_general(
            cot[...], hidden[...], (((0,), (0,)), ((), ())), preferred_element_type=F32
        ).reshape(zs, NY, NC, w, ff)
        early = pl.program_id(0) * zs < NZ // 2
        for i in range(NY):
            yr = lax.rem(i - y + NY, NY)
            first = jnp.where(yr == 1, 2, jnp.where(yr == 2, 0, 1))
            last = jnp.where(yr == 1, 0, jnp.where(yr == 2, 1, 2))
            slot = jnp.where(yr == 0, 3, jnp.where(early, first, last))
            for j in range(zs):
                zero, one = tile_term[j, i, 0], tile_term[j, i, 1]
                keep[slot, j] = jnp.where(c == 0, zero, one).astype(BF)
                give[slot, j] = jnp.where(c == 0, one, zero).astype(BF)

    def out_index(i, where):
        return (0, i, 0, 0)

    return pl.pallas_call(
        body,
        grid_spec=pltpu.PrefetchScalarGridSpec(
            num_scalar_prefetch=1,
            grid=(NZ // zs,),
            in_specs=[
                pl.BlockSpec((n, tile), lambda i, where: (0, i)),
                pl.BlockSpec((n, ff), lambda i, where: (0, 0)),
            ],
            out_specs=[
                pl.BlockSpec((NY, zs, w, ff), out_index),
                pl.BlockSpec((NY, zs, w, ff), out_index),
            ],
        ),
        out_shape=[
            jax.ShapeDtypeStruct((NY, NZ, w, ff), BF),
            jax.ShapeDtypeStruct((NY, NZ, w, ff), BF),
        ],
        compiler_params=pltpu.CompilerParams(
            dimension_semantics=("arbitrary",), vmem_limit_bytes=24 * 1024 * 1024
        ),
        cost_estimate=pl.CostEstimate(
            flops=2 * n * d * ff, bytes_accessed=12 * 1024 * 1024, transcendentals=0
        ),
        name="grad_term",
    )(where, cot, hidden)


def partial_products(where, hidden, own, other):
    parts, rows, ff = hidden.shape
    count = len(own)
    w = own[0][0].shape[1]
    tile = NY * NC * w
    d = count * tile
    pieces, places = [], []
    for cr, blocks in enumerate((own, other)):
        for zr, block in enumerate(blocks):
            yr = 0
            for piece in block:
                places.append((zr, cr, yr))
                pieces.append(piece)
                yr += piece.shape[0]
    n = len(pieces)

    def body(where, hidden, *refs):
        blocks = refs[:n]
        outs, whole = refs[n : n + parts], refs[n + parts]
        ordered, weight, sems = refs[n + parts + 1 :]
        step = pl.program_id(0)
        y, c, t = where[1], where[2], where[3]

        @pl.when(step == 0)
        def _():
            for block, (zr, cr, first) in zip(blocks, places):

                def send(j, _, block=block, zr=zr, cr=cr, first=first):
                    yr = first + j
                    pltpu.make_async_copy(
                        block.at[j],
                        weight.at[zr, lax.rem(y + yr, NY), lax.rem(c + cr, NC)],
                        sems.at[zr, cr, yr],
                    ).start()
                    return 0

                lax.fori_loop(0, block.shape[0], send, 0)
            for i in range(parts):
                ordered[pl.ds(i * rows, rows), :] = hidden[lax.rem(t + i, parts)]

        for cr in range(NC):
            for yr in range(NY):
                pltpu.make_async_copy(
                    blocks[0].at[0], weight.at[step, yr, cr], sems.at[step, cr, yr]
                ).wait()

        part = lax.dot_general(
            ordered[...],
            weight[step].reshape(tile, ff),
            (((1,), (1,)), ((), ())),
            preferred_element_type=F32,
        ).astype(BF)
        for i in range(parts):
            outs[i][...] = part[i * rows : (i + 1) * rows]
        whole[0] = weight[step]

    def at(i, where):
        return lax.rem(i + where[0], NZ)

    return pl.pallas_call(
        body,
        grid_spec=pltpu.PrefetchScalarGridSpec(
            num_scalar_prefetch=1,
            grid=(count,),
            in_specs=[pl.BlockSpec((parts, rows, ff), lambda i, where: (0, 0, 0))]
            + [pl.BlockSpec(memory_space=pltpu.HBM)] * n,
            out_specs=[pl.BlockSpec((rows, tile), lambda i, where: (0, at(i, where)))]
            * parts
            + [
                pl.BlockSpec(
                    (1, NY, NC, w, ff), lambda i, where: (at(i, where), 0, 0, 0, 0)
                )
            ],
            scratch_shapes=[
                pltpu.VMEM((parts * rows, ff), BF),
                pltpu.VMEM((count, NY, NC, w, ff), BF),
                pltpu.SemaphoreType.DMA((count, NC, NY)),
            ],
        ),
        out_shape=[jax.ShapeDtypeStruct((rows, d), BF)] * parts
        + [jax.ShapeDtypeStruct((count, NY, NC, w, ff), BF)],
        compiler_params=pltpu.CompilerParams(
            dimension_semantics=("arbitrary",), vmem_limit_bytes=24 * 1024 * 1024
        ),
        cost_estimate=pl.CostEstimate(
            flops=2 * parts * rows * d * ff,
            bytes_accessed=16 * 1024 * 1024,
            transcendentals=0,
        ),
        name="partial_products",
    )(where, hidden, *pieces)


def pick(x, i, n):
    return lax.dynamic_index_in_dim(x, i % n, 0, keepdims=False)


def shift(x, dz=0, dy=0, dc=0):
    perm = [
        (fs_id(z, y, c), fs_id(z + dz, y + dy, c + dc))
        for z in range(NZ)
        for y in range(NY)
        for c in range(NC)
    ]
    return lax.ppermute(x, "fs", perm)


def shift_x(x, d):
    return lax.ppermute(x, "tp", [(i, (i + d) % NX) for i in range(NX)])


def step(
    later_gate, later_up, early_gate, early_up, early_cotangent, down_weight, grad_running
):
    k = lax.axis_index("fs")
    t = lax.axis_index("tp")
    where = jnp.stack([k // (NY * NC), (k // NC) % NY, k % NC, t]).astype(jnp.int32)
    rows, d = early_cotangent.shape
    ff, _ = down_weight.shape

    h = rows // 2
    cot = early_cotangent
    from_m = shift_x(cot, 1)
    from_p = shift_x(cot, -1)
    far_top = shift_x(from_m[:h], 1)
    far_bot = shift_x(from_p[h:], -1)
    cot_rows = jnp.zeros((NX, rows, d), BF)

    def put(buf, x, i, j=0):
        return lax.dynamic_update_slice(buf, x[None], ((t + i) % NX, j, 0))

    cot_rows = put(cot_rows, cot, 0)
    cot_rows = put(cot_rows, from_p, 1)
    cot_rows = put(cot_rows, from_m, 3)
    cot_rows = put(cot_rows, far_top, 2)
    cot_rows = put(cot_rows, far_bot, 2, h).reshape(NX * rows, d)

    later_hidden = (
        jax.nn.silu(later_gate.astype(F32)) * later_up.astype(F32)
    ).astype(BF)
    gate_value = early_gate.astype(F32)
    up_value = early_up.astype(F32)
    sigma = jax.nn.sigmoid(gate_value)
    early = lax.optimization_barrier((early_gate, early_up))
    early_hidden = (jax.nn.silu(early[0].astype(F32)) * early[1].astype(F32)).astype(BF)

    w0 = down_weight.T
    wy = jnp.stack([w0, shift(w0, dy=-1), shift(w0, dy=2), shift(w0, dy=1)])
    up1, dn1 = shift(wy, dz=1), shift(wy, dz=-1)
    c0 = shift(wy, dc=1)
    up2, dn2 = shift(up1, dz=1), shift(dn1, dz=-1)
    c1, c7 = shift(dn1, dc=1), shift(up1, dc=1)

    give, keep = grad_term(where, cot_rows, early_hidden)
    came = shift(give, dc=1)
    up_y, dn_y, fwd_y, own_y = (
        keep[i].astype(F32) + came[i].astype(F32) for i in range(NY)
    )

    up3, dn3 = shift(up2, dz=1), shift(dn2, dz=-1)
    c2, c6 = shift(dn2, dc=1), shift(up2, dc=1)

    q = NZ // 2
    up = shift(up_y.astype(BF), dy=1)
    dn = shift(dn_y.astype(BF), dy=-1)

    far_u, far_d = shift(up3[:2], dz=1), shift(dn3[2:], dz=-1)
    c3, c5 = shift(dn3, dc=1), shift(up3, dc=1)
    far = jnp.concatenate([far_u, far_d])
    c4 = shift(far, dc=1)
    own = [[wy], [dn1], [dn2], [dn3], [far], [up3], [up2], [up1]]
    other = [[c0], [c1], [c2], [c3], [c4], [c5], [c6], [c7]]

    up2y = shift((fwd_y[:q] + up[:q].astype(F32)).astype(BF), dy=1)
    dn2y = shift((fwd_y[q:] + dn[q:].astype(F32)).astype(BF), dy=-1)
    first = own_y[:q] + dn[:q].astype(F32) + up2y.astype(F32)
    last = own_y[q:] + up[q:].astype(F32) + dn2y.astype(F32)
    reduced = jnp.concatenate([first, last]).astype(BF)
    summed = pick(reduced, where[0], NZ).astype(F32)
    for i in (4, 3, 5, 2, 6, 1, 7):
        block = pick(reduced, where[0] + i, NZ)
        summed = summed + shift(block, dz=i).astype(F32)
    grad_total = grad_running + summed.T

    p0, p1, p2, p3, whole = partial_products(
        where, later_hidden.reshape(NX, rows, ff), own, other
    )
    total = p0.astype(F32)
    for i, p in ((2, p2), (1, p1), (3, p3)):
        total = total + shift_x(p, i).astype(F32)
    mixed = total.astype(BF)

    hidden_cot = jnp.dot(
        cot_rows, whole.reshape(d, ff), preferred_element_type=F32
    )
    gate_grad = (
        hidden_cot * up_value * sigma * (1.0 + gate_value * (1.0 - sigma))
    ).astype(BF)
    up_grad = (hidden_cot * gate_value * sigma).astype(BF)
    return (mixed, gate_grad, up_grad, grad_total)


def solution(mesh):
    placed = (
        P("fs", "tp"),
        P("fs", "tp"),
        P("fs", "tp"),
        P("fs", "tp"),
        P(("fs", "tp"), None),
        P("tp", "fs"),
        P("tp", "fs"),
    )
    return jax.shard_map(
        step,
        mesh=mesh,
        in_specs=placed,
        out_specs=(P(("fs", "tp"), None), P("fs", "tp"), P("fs", "tp"), P("tp", "fs")),
        check_vma=False,
    )
```
